32 devices in a mesh: dp: 4 (over y, x), kv: 4 (over z), tp: 2 (over core).
Axes of the slice: x: 2, y: 2, z: 4, core: 2. Of those that a mesh axis runs over, the one named last changes fastest.
Arguments:
- tokens: bfloat16 [16, 4096], P('dp', ('kv', 'tp')), may hold values from -75 to 75, as said below
- attn_gain: bfloat16 [4096], P('kv'), may hold values from 0.099609375 to 1.8984375
- w_query: bfloat16 [4096, 2048], P('kv', 'tp'), may hold values from -0.09375 to 0.09375
- w_key: bfloat16 [4096, 256], P('kv', 'tp'), may hold values from -0.75 to 0.75
- w_value: bfloat16 [4096, 256], P('kv', 'tp'), may hold values from -0.09375 to 0.09375
- key_cache: bfloat16 [16, 8192, 2, 128], P('dp', 'kv', 'tp'), may hold values from -700 to 700
- value_cache: bfloat16 [16, 8192, 2, 128], P('dp', 'kv', 'tp'), may hold values from -6 to 6
- lam: float32 [16], P('tp'), may hold values from 0.3 to 0.8
- head_gain: bfloat16 [128], replicated, may hold values from 0.099609375 to 1.8984375
- w_out: bfloat16 [2048, 4096], P('tp', 'kv'), may hold values from -0.125 to 0.125
- ffn_gain: bfloat16 [4096], replicated, may hold values from 0.099609375 to 1.8984375
- w_up: bfloat16 [4096, 16384], P(None, ('dp', 'kv', 'tp')), may hold values from -0.09375 to 0.09375
- w_down: bfloat16 [16384, 4096], P(('dp', 'kv', 'tp')), may hold values from -0.09375 to 0.09375
Outputs:
- updated: bfloat16 [16, 4096], P('dp', ('kv', 'tp'))
The draws below stay inside these ranges and needn't reach their ends.
Inputs may be any that keep to these rules, and one draw needn't show every extreme that they name: `tokens`: column scales differ across the width.
All inputs are finite; a program needn't handle non-finite values.
Results may differ from the reference program's by a relative error of at most 0.017.
Values may be sent and summed in bfloat16 or wider, within the bound.
A program may use at most 64 MiB of HBM per device.

```python
import math
import jax
import jax.numpy as jnp
from jax import lax

D = 4096
HEADS = 16
KV_HEADS = 2
HD = 64
VD = 128
FF = 16384
SEQ_DEV = 4
POS_DEV = 2048
BATCH = 16
LENGTH = 8192
N_DP = 4
N_KV = 4
N_TP = 2


def draw_tokens(key, part):
    batch = SEQ_DEV * N_DP
    first, second = jax.random.split(key, 2)
    rough = jax.random.uniform(second, (D,), jnp.float32, 0.7, 1.4)
    column = jnp.exp(jnp.linspace(0.0, math.log(3.5), D)).astype(jnp.float32)
    base = jnp.clip(jax.random.normal(first, (batch, D), jnp.float32), -5.0, 5.0)
    return (base * column * rough).astype(jnp.bfloat16)


def draw_key_cache(key, part):
    batch = SEQ_DEV * N_DP
    length = POS_DEV * N_KV
    wide = 2 * HD
    keys = jax.random.split(key, 1)
    base = jnp.clip(jax.random.normal(keys[0], (batch, length, KV_HEADS, wide), jnp.float32), -6.0, 6.0) * 1.75
    return base.astype(jnp.bfloat16)


def with_spikes(values, own_key, source, target, shards_of, factor):
    def block_of(axis_at):
        return (jnp.arange(values.shape[axis_at]) // (values.shape[axis_at] // shards_of)).reshape((-1,) + (1,) * (values.ndim - 1 - axis_at))

    first = jax.random.permutation(own_key, shards_of)[block_of(target)]
    second = (block_of(target) + shards_of // 2) % shards_of
    return jnp.where((block_of(source) == first) | (block_of(source) == second), factor * values, values)


def shard_levels(stream_key, dims, shards, smallest, largest):
    factor_of, own = 1.0, jax.random.fold_in(stream_key, 6)
    for dim, blocks in shards:
        heights = jnp.exp(jax.random.uniform(jax.random.fold_in(own, dim), (blocks,), jnp.float32, smallest / len(shards), largest / len(shards)))
        factor_of = factor_of * jnp.repeat(heights, dims[dim] // blocks).reshape([-1 if axis == dim else 1 for axis in range(len(dims))])
    return factor_of


def gaussian(stream_key, extent, spread, most, shards=(), held_as=jnp.bfloat16):
    values = spread * jax.random.normal(stream_key, extent, jnp.float32)
    if shards:
        values = values * shard_levels(stream_key, extent, shards, -0.22, 0.18)
    return jnp.clip(values, -most, most).astype(held_as)


def bell_draw_with(key, dims, deviation, most, pieces, heavy, kind=jnp.bfloat16):
    entries = deviation * jax.random.normal(key, dims, jnp.float32)
    if pieces:
        entries = entries * shard_levels(key, dims, pieces, -0.22, 0.18)
    return jnp.clip(with_spikes(entries, jax.random.fold_in(key, 3), *heavy), -most, most).astype(kind)


def setup_inputs(seed: int = 0) -> dict:
    key_list = jax.random.split(jax.random.key(seed), 14)
    tokens = draw_tokens(jax.random.fold_in(key_list[13], 71), 0)
    attn_gain = jnp.clip(1.0 + 0.18 * jax.random.normal(key_list[1], (D,), jnp.float32), 0.099609375, 1.8984375).astype(jnp.bfloat16)
    w_query = gaussian(key_list[2], (D, HEADS * 2 * HD), D ** -0.5, 0.09375, ((0, 4), (1, 2)))
    w_key = gaussian(key_list[3], (D, KV_HEADS * 2 * HD), (D // 64) ** -0.5, 0.75, ((0, 4), (1, 2)))
    w_value = gaussian(key_list[4], (D, KV_HEADS * VD), D ** -0.5, 0.09375, ((0, 4), (1, 2)))
    key_cache = draw_key_cache(jax.random.fold_in(key_list[13], 71), 0)
    value_cache = gaussian(key_list[6], (BATCH, LENGTH, KV_HEADS, VD), 1.0, 6.0, ((0, 4), (1, 4), (2, 2)))
    lam = jnp.clip(0.3 + 0.5 * jax.random.uniform(key_list[7], (HEADS,), jnp.float32) ** shard_levels(key_list[7], (HEADS,), ((0, 2),), -0.2, 0.2), 0.3, 0.8)
    head_gain = jnp.clip(1.0 + 0.18 * jax.random.normal(key_list[8], (VD,), jnp.float32), 0.099609375, 1.8984375).astype(jnp.bfloat16)
    w_out = gaussian(key_list[9], (HEADS * VD, D), (HEADS * VD) ** -0.5, 0.125, ((0, 2), (1, 4)))
    ffn_gain = jnp.clip(1.0 + 0.18 * jax.random.normal(key_list[10], (D,), jnp.float32), 0.099609375, 1.8984375).astype(jnp.bfloat16)
    w_up = gaussian(key_list[11], (D, FF), D ** -0.5, 0.09375, ((1, 32),))
    w_down = bell_draw_with(key_list[12], (FF, D), FF ** -0.5, 0.09375, ((0, 32),), (0, 1, 32, 2.75))
    return {"tokens": tokens, "attn_gain": attn_gain, "w_query": w_query, "w_key": w_key, "w_value": w_value, "key_cache": key_cache, "value_cache": value_cache, "lam": lam, "head_gain": head_gain, "w_out": w_out, "ffn_gain": ffn_gain, "w_up": w_up, "w_down": w_down}


EPS = 1e-06
THETA = 500000.0
OUT_SCALE = 0.8

def settle(value):
    return lax.optimization_barrier(value.astype(jnp.bfloat16)).astype(jnp.float32)

def rotate(value, position):
    half = value.shape[-1] // 2
    inverse = THETA ** (-jnp.arange(half, dtype=jnp.float32) * 2.0 / value.shape[-1])
    angle = position * inverse
    cosine = jnp.cos(angle)
    sine = jnp.sin(angle)
    first = value[..., :half]
    second = value[..., half:]
    return jnp.concatenate([first * cosine - second * sine, second * cosine + first * sine], axis=-1)

def reference(tokens, attn_gain, w_query, w_key, w_value, key_cache, value_cache, lam, head_gain, w_out, ffn_gain, w_up, w_down):
    f32 = jnp.float32
    bf = jnp.bfloat16
    batch = tokens.shape[0]
    length = key_cache.shape[1]
    group = HEADS // KV_HEADS
    scale = HD ** (-0.5)
    xf = tokens.astype(f32)
    inv_rms = lax.rsqrt(lax.optimization_barrier(jnp.mean(xf * xf, axis=-1, keepdims=True)) + EPS)
    scaled = (xf * attn_gain.astype(f32)).astype(bf)
    q_raw = jnp.dot(scaled, w_query, preferred_element_type=f32) * inv_rms
    k_raw = jnp.dot(scaled, w_key, preferred_element_type=f32) * inv_rms
    v_raw = jnp.dot(scaled, w_value, preferred_element_type=f32) * inv_rms
    position = jnp.asarray(length, f32)
    query = settle(rotate(q_raw.reshape(batch, KV_HEADS, group, 2, HD), position))
    new_key = settle(rotate(k_raw.reshape(batch, KV_HEADS, 2, HD), position))
    new_value = settle(v_raw.reshape(batch, KV_HEADS, VD))
    own_score = jnp.einsum('bkgmd,bkmd->bkgm', query, new_key) * scale

    def one_sequence(items):
        query_b, keys_b, values_b, own_b, newval_b = items
        keys_f = keys_b.reshape(length, KV_HEADS, 2, HD).astype(f32)
        scores = jnp.einsum('kgmd,lkmd->kgml', query_b, keys_f) * scale
        top = jnp.maximum(lax.optimization_barrier(jnp.max(scores, axis=-1)), own_b)
        expo = jnp.exp(scores - top[..., None])
        own_w = jnp.exp(own_b - top)
        den = lax.optimization_barrier(jnp.sum(expo, axis=-1)) + own_w
        num = jnp.einsum('kgml,lkv->kgmv', settle(expo), values_b.astype(f32))
        num = num + settle(own_w)[..., None] * newval_b[:, None, None, :]
        return (num, den)
    num, den = lax.map(one_sequence, (query, key_cache, value_cache, own_score, new_value))
    lam_h = lam.astype(f32).reshape(KV_HEADS, group)
    mix = num[..., 0, :] / den[..., 0, None] - lam_h[None, :, :, None] * num[..., 1, :] / den[..., 1, None]
    normed = mix * lax.rsqrt(lax.optimization_barrier(jnp.mean(mix * mix, axis=-1, keepdims=True)) + EPS) * head_gain.astype(f32) * OUT_SCALE
    attended = normed.astype(bf).reshape(batch, N_TP, HEADS * VD // N_TP).astype(f32)
    out_parts = jnp.einsum('btk,tkd->btd', attended, w_out.reshape(N_TP, HEADS * VD // N_TP, D).astype(f32))
    branch = lax.optimization_barrier(jnp.sum(settle(out_parts), axis=1))
    hidden = lax.optimization_barrier((xf + branch).astype(bf))
    hf = hidden.astype(f32)
    inv_two = lax.rsqrt(lax.optimization_barrier(jnp.mean(hf * hf, axis=-1, keepdims=True)) + EPS)
    normed_two = (hf * inv_two * ffn_gain.astype(f32)).astype(bf)
    upward = jnp.dot(normed_two, w_up, preferred_element_type=f32)
    act = jnp.square(jax.nn.relu(upward)).astype(bf)
    down = jnp.dot(act, w_down, preferred_element_type=f32)
    return (hf + down).astype(bf)
```

```python
import functools

import jax
import jax.numpy as jnp
import numpy as np
from jax import lax
from jax.experimental import pallas as pl
from jax.experimental.pallas import tpu as pltpu
from jax.sharding import PartitionSpec as P

HD = 64
VD = 128

EPS = 1e-06
THETA = 500000.0
OUT_SCALE = 0.8
MESH = pl.DeviceIdType.MESH
F32 = jnp.float32
BF = jnp.bfloat16


def rope_table(position):
    half = HD // 2
    inverse = THETA ** (-np.arange(half, dtype=np.float64) * 2.0 / HD)
    angle = position * inverse
    cosine = np.tile(np.cos(angle), 4)
    sine = np.tile(np.concatenate([-np.sin(angle), np.sin(angle)]), 2)
    return np.stack([cosine, sine]).astype(np.float32)


def rotate(value, table):
    half = HD // 2
    lane = lax.broadcasted_iota(jnp.int32, value.shape, 1)
    swapped = jnp.where(
        lane % HD < half, pltpu.roll(value, VD - half, 1), pltpu.roll(value, half, 1)
    )
    return value * table[0:1, :] + swapped * table[1:2, :]


def kernel(
    dims,
    tok,
    gain,
    lam,
    head_gain,
    ffn_gain,
    table,
    wq,
    wk,
    wv,
    kc,
    vc,
    wo,
    wu,
    wd,
    out,
    wq_v,
    wk_v,
    wv_v,
    kc_v,
    vc_v,
    wo_v,
    wu_v,
    wd_v,
    slab,
    part,
    q_rows,
    k_rows,
    o_part,
    s_part,
    att,
    half_out,
    half_in,
    hid,
    grid,
    down_out,
    down_in,
    load_sem,
    slab_sem,
    part_sem,
    o_sem,
    s_sem,
    half_sem,
    hid_sem,
    down_sem,
):
    n_dp, n_kv, n_tp = dims
    n = n_dp * n_kv * n_tp
    blocks = n_kv * n_tp
    rows, width = tok.shape
    heads = lam.shape[0]
    q_cols = heads * VD
    model = blocks * width
    scale = HD ** (-0.5)
    i_dp, i_kv, i_tp = lax.axis_index("dp"), lax.axis_index("kv"), lax.axis_index("tp")
    me = (i_dp * n_kv + i_kv) * n_tp + i_tp

    def device(p):
        return (p // blocks, (p // n_tp) % n_kv, p % n_tp)

    loads = [
        pltpu.make_async_copy(src, dst, load_sem.at[k])
        for k, (src, dst) in enumerate(
            (
                (wq, wq_v),
                (wk, wk_v),
                (wv, wv_v),
                (kc, kc_v),
                (vc, vc_v),
                (wo, wo_v),
                (wu, wu_v),
                (wd, wd_v),
            )
        )
    ]
    for load in loads:
        load.start()

    barrier = pltpu.get_barrier_semaphore()

    def greet(i, carry):
        pl.semaphore_signal(
            barrier, inc=1, device_id=device((me + i) % n), device_id_type=MESH
        )
        return carry

    lax.fori_loop(1, n, greet, 0)
    pl.semaphore_wait(barrier, n - 1)

    def to_tp(i, src, dst, sem):
        peer = (i_tp + i) % n_tp
        return pltpu.make_async_remote_copy(
            src_ref=src(peer),
            dst_ref=dst.at[i_tp],
            send_sem=sem.at[0, peer],
            recv_sem=sem.at[1, i_tp],
            device_id=(i_dp, i_kv, peer),
            device_id_type=MESH,
        )

    def from_tp(i, dst, sem):
        peer = (i_tp + i) % n_tp
        return pltpu.make_async_remote_copy(
            src_ref=dst.at[peer],
            dst_ref=dst.at[peer],
            send_sem=sem.at[0, peer],
            recv_sem=sem.at[1, peer],
            device_id=(i_dp, i_kv, peer),
            device_id_type=MESH,
        )

    def to_kv(i, dst, sem):
        peer = (i_kv + i) % n_kv
        return pltpu.make_async_remote_copy(
            src_ref=dst.at[i_kv],
            dst_ref=dst.at[i_kv],
            send_sem=sem.at[0, peer],
            recv_sem=sem.at[1, i_kv],
            device_id=(i_dp, peer, i_tp),
            device_id_type=MESH,
        )

    def from_kv(i, dst, sem):
        peer = (i_kv + i) % n_kv
        return pltpu.make_async_remote_copy(
            src_ref=dst.at[peer],
            dst_ref=dst.at[peer],
            send_sem=sem.at[0, peer],
            recv_sem=sem.at[1, peer],
            device_id=(i_dp, peer, i_tp),
            device_id_type=MESH,
        )

    def to_all(i, src, dst, sem):
        peer = (me + i) % n
        return pltpu.make_async_remote_copy(
            src_ref=src(peer),
            dst_ref=dst.at[me],
            send_sem=sem.at[0, peer],
            recv_sem=sem.at[1, me],
            device_id=device(peer),
            device_id_type=MESH,
        )

    def from_all(i, dst, sem):
        peer = (me + i) % n
        return pltpu.make_async_remote_copy(
            src_ref=dst.at[peer],
            dst_ref=dst.at[peer],
            send_sem=sem.at[0, peer],
            recv_sem=sem.at[1, peer],
            device_id=device(peer),
            device_id_type=MESH,
        )

    def each(count, act):
        def step(i, carry):
            act(i)
            return carry

        lax.fori_loop(1, count, step, 0)

    for i in range(1, n_tp):
        to_tp(i, lambda peer: tok, slab, slab_sem).start()
    slab[i_tp] = tok[...]
    for load in loads[:3]:
        load.wait()
    for i in range(1, n_tp):
        from_tp(i, slab, slab_sem).wait_recv()

    part_q = jnp.zeros((rows, q_cols), F32)
    part_k = jnp.zeros((rows, VD), F32)
    part_v = jnp.zeros((rows, VD), F32)
    local_sq = jnp.zeros((rows, 1), F32)
    for t in range(n_tp):
        span = slice(t * width, (t + 1) * width)
        value = slab[t].astype(F32)
        local_sq += jnp.sum(value * value, axis=-1, keepdims=True)
        scaled = (value * gain[:, span].astype(F32)).astype(BF)
        part_q += jnp.dot(scaled, wq_v[span, :], preferred_element_type=F32)
        part_k += jnp.dot(scaled, wk_v[span, :], preferred_element_type=F32)
        part_v += jnp.dot(scaled, wv_v[span, :], preferred_element_type=F32)
    part[i_kv, :, 0:q_cols] = part_q
    part[i_kv, :, q_cols : q_cols + VD] = part_k
    part[i_kv, :, q_cols + VD : q_cols + 2 * VD] = part_v
    part[i_kv, :, q_cols + 2 * VD : q_cols + 3 * VD] = jnp.broadcast_to(local_sq, (rows, VD))
    each(n_kv, lambda i: to_kv(i, part, part_sem).start())
    each(n_kv, lambda i: from_kv(i, part, part_sem).wait_recv())

    total = part[0]
    for k in range(1, n_kv):
        total += part[k]
    inv_rms = lax.rsqrt(total[:, q_cols + 2 * VD : q_cols + 2 * VD + 1] / model + EPS)
    table_v = table[...]
    for h in range(heads):
        chunk = total[:, h * VD : (h + 1) * VD] * inv_rms
        for r in range(rows):
            q_rows[r, h : h + 1, :] = chunk[r : r + 1, :]
    k_rows[...] = jnp.zeros_like(k_rows)
    k_rows[0:rows, :] = total[:, q_cols : q_cols + VD] * inv_rms
    new_key = rotate(k_rows[...], table_v).astype(BF).astype(F32)
    new_value = (total[:, q_cols + VD : q_cols + 2 * VD] * inv_rms).astype(BF).astype(F32)

    for load in loads[3:5]:
        load.wait()
    pairs = 2 * heads
    lane_h = lax.broadcasted_iota(jnp.int32, (heads, VD), 1)
    lane_p = lax.broadcasted_iota(jnp.int32, (pairs, VD), 1)
    row_p = lax.broadcasted_iota(jnp.int32, (pairs, VD), 0)
    own_scores = []
    stat_row = jnp.zeros((1, VD), F32)
    for r in range(rows):
        query = rotate(q_rows[r], table_v).astype(BF).astype(F32)
        both = jnp.concatenate(
            [jnp.where(lane_h < HD, query, 0.0), jnp.where(lane_h < HD, 0.0, query)], axis=0
        )
        own_scores.append(
            jnp.sum(both * new_key[r : r + 1, :], axis=-1, keepdims=True) * scale
        )
        scores = (
            lax.dot_general(
                both.astype(BF), kc_v[r], (((1,), (1,)), ((), ())), preferred_element_type=F32
            )
            * scale
        )
        top = jnp.max(scores, axis=-1, keepdims=True)
        expo = jnp.exp(scores - top)
        den = jnp.sum(expo, axis=-1, keepdims=True)
        num = jnp.dot(expo.astype(BF), vc_v[r], preferred_element_type=F32)
        o_part[i_kv, r] = (num / den).astype(BF)
        stat = top + jnp.log(den)
        stat_row += jnp.sum(
            jnp.where(lane_p == row_p + r * pairs, stat, 0.0), axis=0, keepdims=True
        )
    s_part[i_kv] = jnp.broadcast_to(stat_row, (8, VD))
    each(n_kv, lambda i: to_kv(i, s_part, s_sem).start())
    each(n_kv, lambda i: to_kv(i, o_part, o_sem).start())
    each(n_kv, lambda i: from_kv(i, s_part, s_sem).wait_recv())
    each(n_kv, lambda i: from_kv(i, o_part, o_sem).wait_recv())

    lam_h = lam[...]
    for r in range(rows):
        own = own_scores[r]
        stats = []
        top = own
        for k in range(n_kv):
            stat = jnp.sum(
                jnp.where(lane_p == row_p + r * pairs, s_part[k][0:1, :], 0.0),
                axis=-1,
                keepdims=True,
            )
            stats.append(stat)
            top = jnp.maximum(top, stat)
        own_weight = jnp.exp(own - top)
        den = own_weight
        num = own_weight * new_value[r : r + 1, :]
        for k in range(n_kv):
            weight = jnp.exp(stats[k] - top)
            den += weight
            num += weight * o_part[k, r].astype(F32)
        ratio = num / den
        mix = ratio[0:heads, :] - lam_h * ratio[heads:, :]
        normed = (
            mix
            * lax.rsqrt(jnp.mean(mix * mix, axis=-1, keepdims=True) + EPS)
            * head_gain[...].astype(F32)
            * OUT_SCALE
        )
        for h in range(heads):
            att[r : r + 1, h * VD : (h + 1) * VD] = normed[h : h + 1, :]

    loads[5].wait()
    part_out = jnp.dot(att[...].astype(BF), wo_v[...], preferred_element_type=F32)
    for t in range(n_tp):
        half_out[t] = part_out[:, t * width : (t + 1) * width].astype(BF)
    for i in range(1, n_tp):
        to_tp(i, lambda peer: half_out.at[peer], half_in, half_sem).start()
    half_in[i_tp] = half_out[i_tp]
    for i in range(1, n_tp):
        from_tp(i, half_in, half_sem).wait_recv()
    branch = half_in[0].astype(F32)
    for t in range(1, n_tp):
        branch += half_in[t].astype(F32)
    hidden = (tok[...].astype(F32) + branch).astype(BF)
    hid[me] = hidden
    each(n, lambda i: to_all(i, lambda peer: hid.at[me], hid, hid_sem).start())
    each(n, lambda i: from_all(i, hid, hid_sem).wait_recv())

    row_sq = jnp.zeros((n_dp * rows, 1), F32)
    for c in range(blocks):
        for a in range(n_dp):
            grid[c, a * rows : (a + 1) * rows, :] = hid[a * blocks + c].astype(F32)
        value = grid[c]
        row_sq += jnp.sum(value * value, axis=-1, keepdims=True)
    inv_two = lax.rsqrt(row_sq / model + EPS)
    loads[6].wait()
    upward = jnp.zeros((n_dp * rows, wu_v.shape[1]), F32)
    for c in range(blocks):
        span = slice(c * width, (c + 1) * width)
        normed_two = (grid[c] * inv_two * ffn_gain[:, span].astype(F32)).astype(BF)
        upward += jnp.dot(normed_two, wu_v[span, :], preferred_element_type=F32)
    act = jnp.square(jnp.maximum(upward, 0.0)).astype(BF)
    loads[7].wait()
    for c in range(blocks):
        span = slice(c * width, (c + 1) * width)
        down = jnp.dot(act, wd_v[:, span], preferred_element_type=F32)
        for a in range(n_dp):
            down_out[a * blocks + c] = down[a * rows : (a + 1) * rows, :].astype(BF)
    each(n, lambda i: to_all(i, lambda peer: down_out.at[peer], down_in, down_sem).start())
    down_in[me] = down_out[me]
    each(n, lambda i: from_all(i, down_in, down_sem).wait_recv())
    mixed = down_in[0].astype(F32)
    for p in range(1, n):
        mixed += down_in[p].astype(F32)
    out[...] = (hidden.astype(F32) + mixed).astype(BF)

    for i in range(1, n_tp):
        to_tp(i, lambda peer: tok, slab, slab_sem).wait_send()
        to_tp(i, lambda peer: half_out.at[peer], half_in, half_sem).wait_send()
    for dst, sem in ((part, part_sem), (s_part, s_sem), (o_part, o_sem)):
        each(n_kv, lambda i: to_kv(i, dst, sem).wait_send())
    each(n, lambda i: to_all(i, lambda peer: hid.at[me], hid, hid_sem).wait_send())
    each(n, lambda i: to_all(i, lambda peer: down_out.at[peer], down_in, down_sem).wait_send())


def local(
    dims,
    tokens,
    attn_gain,
    w_query,
    w_key,
    w_value,
    key_cache,
    value_cache,
    lam,
    head_gain,
    w_out,
    ffn_gain,
    w_up,
    w_down,
):
    n_dp, n_kv, n_tp = dims
    n = n_dp * n_kv * n_tp
    blocks = n_kv * n_tp
    rows, width = tokens.shape
    positions = key_cache.shape[1]
    heads = lam.shape[0]
    keys = key_cache.reshape(rows, positions, VD)
    values = value_cache.reshape(rows, positions, VD)
    table = jnp.asarray(rope_table(positions * n_kv))
    vmem = pl.BlockSpec(memory_space=pltpu.VMEM)
    hbm = pl.BlockSpec(memory_space=pl.ANY)
    big = (w_query, w_key, w_value, keys, values, w_out, w_up, w_down)
    dma = pltpu.SemaphoreType.DMA
    return pl.pallas_call(
        functools.partial(kernel, dims),
        name="layer",
        out_shape=jax.ShapeDtypeStruct((rows, width), BF),
        in_specs=[vmem] * 6 + [hbm] * 8,
        out_specs=vmem,
        scratch_shapes=[pltpu.VMEM(a.shape, BF) for a in big]
        + [
            pltpu.VMEM((n_tp, rows, width), BF),
            pltpu.VMEM((n_kv, rows, heads * VD + 3 * VD), F32),
            pltpu.VMEM((rows, heads, VD), F32),
            pltpu.VMEM((8, VD), F32),
            pltpu.VMEM((n_kv, rows, 2 * heads, VD), BF),
            pltpu.VMEM((n_kv, 8, VD), F32),
            pltpu.VMEM((rows, heads * VD), F32),
            pltpu.VMEM((n_tp, rows, width), BF),
            pltpu.VMEM((n_tp, rows, width), BF),
            pltpu.VMEM((n, rows, width), BF),
            pltpu.VMEM((blocks, n_dp * rows, width), F32),
            pltpu.VMEM((n, rows, width), BF),
            pltpu.VMEM((n, rows, width), BF),
            dma((8,)),
            dma((2, n_tp)),
            dma((2, n_kv)),
            dma((2, n_kv)),
            dma((2, n_kv)),
            dma((2, n_tp)),
            dma((2, n)),
            dma((2, n)),
        ],
        compiler_params=pltpu.CompilerParams(
            collective_id=0, has_side_effects=True, vmem_limit_bytes=60 * 1024 * 1024
        ),
    )(
        tokens,
        attn_gain.reshape(1, -1),
        lam.reshape(-1, 1),
        head_gain.reshape(1, -1),
        ffn_gain.reshape(1, -1),
        table,
        *big,
    )


def solution(mesh):
    in_specs = (
        P("dp", ("kv", "tp")),
        P("kv"),
        P("kv", "tp"),
        P("kv", "tp"),
        P("kv", "tp"),
        P("dp", "kv", "tp", None),
        P("dp", "kv", "tp", None),
        P("tp"),
        P(),
        P("tp", "kv"),
        P(),
        P(None, ("dp", "kv", "tp")),
        P(("dp", "kv", "tp"), None),
    )
    out_specs = P("dp", ("kv", "tp"))
    dims = (mesh.shape["dp"], mesh.shape["kv"], mesh.shape["tp"])
    return jax.shard_map(
        functools.partial(local, dims),
        mesh=mesh,
        in_specs=in_specs,
        out_specs=out_specs,
        check_vma=False,
    )
```

```python
import functools

import jax
import jax.numpy as jnp
import numpy as np
from jax import lax
from jax.experimental import pallas as pl
from jax.experimental.pallas import tpu as pltpu
from jax.sharding import PartitionSpec as P

HD = 64
VD = 128

EPS = 1e-06
THETA = 500000.0
OUT_SCALE = 0.8
MESH = pl.DeviceIdType.MESH
F32 = jnp.float32
BF = jnp.bfloat16


def rope_table(position):
    half = HD // 2
    inverse = THETA ** (-np.arange(half, dtype=np.float64) * 2.0 / HD)
    angle = position * inverse
    cosine = np.tile(np.cos(angle), 4)
    sine = np.tile(np.concatenate([-np.sin(angle), np.sin(angle)]), 2)
    return np.stack([cosine, sine]).astype(np.float32)


def rotate(value, table):
    half = HD // 2
    lane = lax.broadcasted_iota(jnp.int32, value.shape, 1)
    swapped = jnp.where(
        lane % HD < half, pltpu.roll(value, VD - half, 1), pltpu.roll(value, half, 1)
    )
    return value * table[0:1, :] + swapped * table[1:2, :]


def kernel(
    dims,
    tok,
    gain,
    lam,
    head_gain,
    ffn_gain,
    table,
    wq,
    wk,
    wv,
    kc,
    vc,
    wo,
    wu,
    wd,
    out,
    wq_v,
    wk_v,
    wv_v,
    kc_v,
    vc_v,
    wo_v,
    wu_v,
    wd_v,
    slab,
    part,
    q_rows,
    k_rows,
    o_part,
    s_part,
    att,
    half_out,
    half_in,
    hid,
    grid,
    gains_two,
    down_out,
    down_in,
    load_sem,
    slab_sem,
    part_sem,
    o_sem,
    s_sem,
    half_sem,
    hid_sem,
    down_sem,
):
    n_dp, n_kv, n_tp = dims
    n = n_dp * n_kv * n_tp
    blocks = n_kv * n_tp
    rows, width = tok.shape
    heads = lam.shape[1]
    q_cols = heads * VD
    model = blocks * width
    scale = HD ** (-0.5)
    i_dp, i_kv, i_tp = lax.axis_index("dp"), lax.axis_index("kv"), lax.axis_index("tp")
    me = (i_dp * n_kv + i_kv) * n_tp + i_tp

    def device(p):
        return (p // blocks, (p // n_tp) % n_kv, p % n_tp)

    def gain_row(ref, c):
        step = width // VD
        return jnp.concatenate(
            [ref[c * step + j : c * step + j + 1, :].astype(F32) for j in range(step)], axis=1
        )

    loads = [
        pltpu.make_async_copy(src, dst, load_sem.at[k])
        for k, (src, dst) in enumerate(
            (
                (wq, wq_v),
                (wk, wk_v),
                (wv, wv_v),
                (kc, kc_v),
                (vc, vc_v),
                (wo, wo_v),
                (wu, wu_v),
                (wd, wd_v),
            )
        )
    ]
    for load in loads:
        load.start()

    barrier = pltpu.get_barrier_semaphore()

    def greet(i, carry):
        pl.semaphore_signal(
            barrier, inc=1, device_id=device((me + i) % n), device_id_type=MESH
        )
        return carry

    lax.fori_loop(1, n, greet, 0)

    gains = [gain_row(gain, t) for t in range(n_tp)]

    def project(t, value):
        value = value.astype(F32)
        row = gains[0]
        for k in range(1, n_tp):
            row = jnp.where(t == k, gains[k], row)
        span = pl.ds(pl.multiple_of(t * width, width), width)
        scaled = (value * row).astype(BF)
        return (
            jnp.dot(scaled, wq_v[span, :], preferred_element_type=F32),
            jnp.dot(scaled, wk_v[span, :], preferred_element_type=F32),
            jnp.dot(scaled, wv_v[span, :], preferred_element_type=F32),
            jnp.sum(value * value, axis=-1, keepdims=True),
        )

    for load in loads[:3]:
        load.wait()
    sums = project(i_tp, tok[...])
    pl.semaphore_wait(barrier, n - 1)

    def to_tp(i, src, dst, sem):
        peer = (i_tp + i) % n_tp
        return pltpu.make_async_remote_copy(
            src_ref=src(peer),
            dst_ref=dst.at[i_tp],
            send_sem=sem.at[0, peer],
            recv_sem=sem.at[1, i_tp],
            device_id=(i_dp, i_kv, peer),
            device_id_type=MESH,
        )

    def from_tp(i, dst, sem):
        peer = (i_tp + i) % n_tp
        return pltpu.make_async_remote_copy(
            src_ref=dst.at[peer],
            dst_ref=dst.at[peer],
            send_sem=sem.at[0, peer],
            recv_sem=sem.at[1, peer],
            device_id=(i_dp, i_kv, peer),
            device_id_type=MESH,
        )

    def to_kv(i, dst, sem):
        peer = (i_kv + i) % n_kv
        return pltpu.make_async_remote_copy(
            src_ref=dst.at[i_kv],
            dst_ref=dst.at[i_kv],
            send_sem=sem.at[0, peer],
            recv_sem=sem.at[1, i_kv],
            device_id=(i_dp, peer, i_tp),
            device_id_type=MESH,
        )

    def from_kv(i, dst, sem):
        peer = (i_kv + i) % n_kv
        return pltpu.make_async_remote_copy(
            src_ref=dst.at[peer],
            dst_ref=dst.at[peer],
            send_sem=sem.at[0, peer],
            recv_sem=sem.at[1, peer],
            device_id=(i_dp, peer, i_tp),
            device_id_type=MESH,
        )

    def to_one(peer, src, dst, sem):
        return pltpu.make_async_remote_copy(
            src_ref=src(peer),
            dst_ref=dst.at[me],
            send_sem=sem.at[0, peer],
            recv_sem=sem.at[1, me],
            device_id=device(peer),
            device_id_type=MESH,
        )

    def to_all(i, src, dst, sem):
        return to_one((me + i) % n, src, dst, sem)

    def arrived(peer, dst, sem):
        pltpu.make_async_remote_copy(
            src_ref=dst.at[peer],
            dst_ref=dst.at[peer],
            send_sem=sem.at[0, peer],
            recv_sem=sem.at[1, peer],
            device_id=device(peer),
            device_id_type=MESH,
        ).wait_recv()

    def each(count, act):
        def step(i, carry):
            act(i)
            return carry

        lax.fori_loop(1, count, step, 0)

    for i in range(1, n_tp):
        to_tp(i, lambda peer: tok, slab, slab_sem).start()
    for i in range(1, n_tp):
        from_tp(i, slab, slab_sem).wait_recv()
        peer = (i_tp + i) % n_tp
        sums = tuple(x + y for x, y in zip(sums, project(peer, slab[peer])))
    part_q, part_k, part_v, local_sq = sums
    part[i_kv, :, 0:q_cols] = part_q.astype(BF)
    part[i_kv, :, q_cols : q_cols + VD] = part_k.astype(BF)
    part[i_kv, :, q_cols + VD : q_cols + 2 * VD] = part_v.astype(BF)
    lane_s = lax.broadcasted_iota(jnp.int32, (rows, VD), 1)
    square = jnp.broadcast_to(local_sq, (rows, VD))
    high = square.astype(BF).astype(F32)
    middle = (square - high).astype(BF).astype(F32)
    low = square - high - middle
    terms = jnp.where(lane_s == 0, high, jnp.where(lane_s == 1, middle, low))
    part[i_kv, :, q_cols + 2 * VD :] = jnp.where(lane_s < 3, terms, 0.0).astype(BF)
    each(n_kv, lambda i: to_kv(i, part, part_sem).start())
    each(n_kv, lambda i: from_kv(i, part, part_sem).wait_recv())

    total = part[0].astype(F32)
    for k in range(1, n_kv):
        total += part[k].astype(F32)
    total_sq = jnp.sum(total[:, q_cols + 2 * VD :], axis=-1, keepdims=True)
    inv_rms = lax.rsqrt(total_sq / model + EPS)
    table_v = table[...]
    for h in range(heads):
        chunk = total[:, h * VD : (h + 1) * VD] * inv_rms
        for r in range(rows):
            q_rows[r, h : h + 1, :] = chunk[r : r + 1, :]
    k_rows[...] = jnp.zeros_like(k_rows)
    k_rows[0:rows, :] = total[:, q_cols : q_cols + VD] * inv_rms
    new_key = rotate(k_rows[...], table_v).astype(BF).astype(F32)
    new_value = (total[:, q_cols + VD : q_cols + 2 * VD] * inv_rms).astype(BF).astype(F32)

    for load in loads[3:5]:
        load.wait()
    pairs = 2 * heads
    lane_h = lax.broadcasted_iota(jnp.int32, (heads, VD), 1)
    lane_p = lax.broadcasted_iota(jnp.int32, (pairs, VD), 1)
    row_p = lax.broadcasted_iota(jnp.int32, (pairs, VD), 0)
    own_scores = []
    stat_row = jnp.zeros((1, VD), F32)
    for r in range(rows):
        query = rotate(q_rows[r], table_v).astype(BF).astype(F32)
        both = jnp.concatenate(
            [jnp.where(lane_h < HD, query, 0.0), jnp.where(lane_h < HD, 0.0, query)], axis=0
        )
        own_scores.append(
            jnp.sum(both * new_key[r : r + 1, :], axis=-1, keepdims=True) * scale
        )
        scores = (
            lax.dot_general(
                both.astype(BF), kc_v[r], (((1,), (1,)), ((), ())), preferred_element_type=F32
            )
            * scale
        )
        top = jnp.max(scores, axis=-1, keepdims=True)
        expo = jnp.exp(scores - top)
        den = jnp.sum(expo, axis=-1, keepdims=True)
        num = jnp.dot(expo.astype(BF), vc_v[r], preferred_element_type=F32)
        o_part[r, i_kv] = (num / den).astype(BF)
        for i in range(1, n_kv):
            to_kv(i, o_part.at[r], o_sem.at[r]).start()
        stat = top + jnp.log(den)
        stat_row += jnp.sum(
            jnp.where(lane_p == row_p + r * pairs, stat, 0.0), axis=0, keepdims=True
        )
    s_part[i_kv] = jnp.broadcast_to(stat_row, (8, VD))
    each(n_kv, lambda i: to_kv(i, s_part, s_sem).start())
    each(n_kv, lambda i: from_kv(i, s_part, s_sem).wait_recv())
    for r in range(rows):
        for i in range(1, n_kv):
            from_kv(i, o_part.at[r], o_sem.at[r]).wait_recv()

    head_row = lax.broadcasted_iota(jnp.int32, (heads, heads), 0)
    head_lane = lax.broadcasted_iota(jnp.int32, (heads, heads), 1)
    for c in range(blocks):
        gains_two[c] = gain_row(ffn_gain, c)
    lam_h = jnp.sum(
        jnp.where(head_row == head_lane, lam[...], 0.0), axis=-1, keepdims=True
    )
    for r in range(rows):
        own = own_scores[r]
        stats = []
        top = own
        for k in range(n_kv):
            stat = jnp.sum(
                jnp.where(lane_p == row_p + r * pairs, s_part[k][0:1, :], 0.0),
                axis=-1,
                keepdims=True,
            )
            stats.append(stat)
            top = jnp.maximum(top, stat)
        own_weight = jnp.exp(own - top)
        den = own_weight
        num = own_weight * new_value[r : r + 1, :]
        for k in range(n_kv):
            weight = jnp.exp(stats[k] - top)
            den += weight
            num += weight * o_part[r, k].astype(F32)
        ratio = num / den
        mix = ratio[0:heads, :] - lam_h * ratio[heads:, :]
        normed = (
            mix
            * lax.rsqrt(jnp.mean(mix * mix, axis=-1, keepdims=True) + EPS)
            * head_gain[...].astype(F32)
            * OUT_SCALE
        )
        for h in range(heads):
            att[r : r + 1, h * VD : (h + 1) * VD] = normed[h : h + 1, :]

    loads[5].wait()
    part_out = jnp.dot(att[...].astype(BF), wo_v[...], preferred_element_type=F32)
    for t in range(n_tp):
        half_out[t] = part_out[:, t * width : (t + 1) * width].astype(BF)
    for i in range(1, n_tp):
        to_tp(i, lambda peer: half_out.at[peer], half_in, half_sem).start()
    half_in[i_tp] = half_out[i_tp]
    for i in range(1, n_tp):
        from_tp(i, half_in, half_sem).wait_recv()
    branch = half_in[0].astype(F32)
    for t in range(1, n_tp):
        branch += half_in[t].astype(F32)
    hidden = (tok[...].astype(F32) + branch).astype(BF)
    hid[me] = hidden
    each(n, lambda i: to_all(i, lambda peer: hid.at[me], hid, hid_sem).start())

    order = sorted(range(n_kv), key=lambda j: min(j, n_kv - j))
    row_sq = jnp.zeros((n_dp * rows, 1), F32)
    upward = jnp.zeros((n_dp * rows, wu_v.shape[1]), F32)
    loads[6].wait()
    for j in order:
        for u in range(n_tp):
            c = ((i_kv + j) % n_kv) * n_tp + (i_tp + u) % n_tp
            for a in range(n_dp):
                p = a * blocks + c
                if j or u:
                    arrived(p, hid, hid_sem)
                else:

                    @pl.when(p != me)
                    def _():
                        arrived(p, hid, hid_sem)

                grid[c, a * rows : (a + 1) * rows, :] = hid[p].astype(F32)
            value = grid[c]
            row_sq += jnp.sum(value * value, axis=-1, keepdims=True)
            span = pl.ds(pl.multiple_of(c * width, width), width)
            upward += jnp.dot(
                (value * gains_two[c]).astype(BF), wu_v[span, :], preferred_element_type=F32
            )
    inv_two = lax.rsqrt(row_sq / model + EPS)
    act = jnp.square(jnp.maximum(upward * inv_two, 0.0)).astype(BF)
    loads[7].wait()
    for j in reversed(order):
        for u in reversed(range(n_tp)):
            c = ((i_kv + j) % n_kv) * n_tp + (i_tp + u) % n_tp
            span = pl.ds(pl.multiple_of(c * width, width), width)
            down = jnp.dot(act, wd_v[:, span], preferred_element_type=F32)
            for a in range(n_dp):
                down_out[a * blocks + c] = down[a * rows : (a + 1) * rows, :].astype(BF)
            for a in reversed(range(n_dp)):
                if j or u or a:
                    to_one(
                        ((i_dp + a) % n_dp) * blocks + c,
                        lambda peer: down_out.at[peer],
                        down_in,
                        down_sem,
                    ).start()
    mixed = down_out[me].astype(F32)
    for j in order:
        for u in range(n_tp):
            for a in range(n_dp):
                if j or u or a:
                    p = ((i_dp + a) % n_dp) * blocks
                    p += ((i_kv + j) % n_kv) * n_tp + (i_tp + u) % n_tp
                    arrived(p, down_in, down_sem)
                    mixed += down_in[p].astype(F32)
    out[...] = (hidden.astype(F32) + mixed).astype(BF)

    for i in range(1, n_tp):
        to_tp(i, lambda peer: tok, slab, slab_sem).wait_send()
        to_tp(i, lambda peer: half_out.at[peer], half_in, half_sem).wait_send()
    each(n_kv, lambda i: to_kv(i, part, part_sem).wait_send())
    each(n_kv, lambda i: to_kv(i, s_part, s_sem).wait_send())
    for r in range(rows):
        for i in range(1, n_kv):
            to_kv(i, o_part.at[r], o_sem.at[r]).wait_send()
    each(n, lambda i: to_all(i, lambda peer: hid.at[me], hid, hid_sem).wait_send())
    each(n, lambda i: to_all(i, lambda peer: down_out.at[peer], down_in, down_sem).wait_send())


def local(
    dims,
    tokens,
    attn_gain,
    w_query,
    w_key,
    w_value,
    key_cache,
    value_cache,
    lam,
    head_gain,
    w_out,
    ffn_gain,
    w_up,
    w_down,
):
    n_dp, n_kv, n_tp = dims
    n = n_dp * n_kv * n_tp
    blocks = n_kv * n_tp
    rows, width = tokens.shape
    positions = key_cache.shape[1]
    heads = lam.shape[0]
    keys = key_cache.reshape(rows, positions, VD)
    values = value_cache.reshape(rows, positions, VD)
    table = jnp.asarray(rope_table(positions * n_kv))
    vmem = pl.BlockSpec(memory_space=pltpu.VMEM)
    hbm = pl.BlockSpec(memory_space=pltpu.HBM)
    big = (w_query, w_key, w_value, keys, values, w_out, w_up, w_down)
    dma = pltpu.SemaphoreType.DMA
    return pl.pallas_call(
        functools.partial(kernel, dims),
        name="layer",
        out_shape=jax.ShapeDtypeStruct((rows, width), BF),
        in_specs=[vmem] * 6 + [hbm] * 8,
        out_specs=vmem,
        scratch_shapes=[pltpu.VMEM(a.shape, BF) for a in big]
        + [
            pltpu.VMEM((n_tp, rows, width), BF),
            pltpu.VMEM((n_kv, rows, heads * VD + 3 * VD), BF),
            pltpu.VMEM((rows, heads, VD), F32),
            pltpu.VMEM((8, VD), F32),
            pltpu.VMEM((rows, n_kv, 2 * heads, VD), BF),
            pltpu.VMEM((n_kv, 8, VD), F32),
            pltpu.VMEM((rows, heads * VD), F32),
            pltpu.VMEM((n_tp, rows, width), BF),
            pltpu.VMEM((n_tp, rows, width), BF),
            pltpu.VMEM((n, rows, width), BF),
            pltpu.VMEM((blocks, n_dp * rows, width), F32),
            pltpu.VMEM((blocks, 1, width), F32),
            pltpu.VMEM((n, rows, width), BF),
            pltpu.VMEM((n, rows, width), BF),
            dma((8,)),
            dma((2, n_tp)),
            dma((2, n_kv)),
            dma((rows, 2, n_kv)),
            dma((2, n_kv)),
            dma((2, n_tp)),
            dma((2, n)),
            dma((2, n)),
        ],
        compiler_params=pltpu.CompilerParams(
            collective_id=0, has_side_effects=True, vmem_limit_bytes=63 * 1024 * 1024
        ),
    )(
        tokens,
        attn_gain.reshape(-1, VD),
        lam.reshape(1, -1),
        head_gain.reshape(1, -1),
        ffn_gain.reshape(-1, VD),
        table,
        *big,
    )


def solution(mesh):
    in_specs = (
        P("dp", ("kv", "tp")),
        P("kv"),
        P("kv", "tp"),
        P("kv", "tp"),
        P("kv", "tp"),
        P("dp", "kv", "tp", None),
        P("dp", "kv", "tp", None),
        P("tp"),
        P(),
        P("tp", "kv"),
        P(),
        P(None, ("dp", "kv", "tp")),
        P(("dp", "kv", "tp"), None),
    )
    out_specs = P("dp", ("kv", "tp"))
    dims = (mesh.shape["dp"], mesh.shape["kv"], mesh.shape["tp"])
    return jax.shard_map(
        functools.partial(local, dims),
        mesh=mesh,
        in_specs=in_specs,
        out_specs=out_specs,
        check_vma=False,
    )
```
